1024 devices in a mesh: rep: 2 (over z_hi), fs: 64 (over z_lo, y), tp: 8 (over x, core).
Axes of the slice: x: 4, y: 8, z: 16 (z_hi: 2, z_lo: 8; z = z_hi * 8 + z_lo), core: 2. Of those that a mesh axis runs over, the one named last changes fastest.
Arguments:
- stream: bfloat16 [32768, 1536], P(('rep', 'fs')), may hold values from -6 to 6
- mix_pre_gain: float32 [1536], replicated, may hold values from 0.1 to 1.9
- w_outer_gate: bfloat16 [1536, 768], P('fs', 'tp'), may hold values from -0.15625 to 0.15625
- w_inner_gate: bfloat16 [1536, 768], P('fs', 'tp'), may hold values from -0.15625 to 0.15625
- w_value: bfloat16 [1536, 768], P('fs', 'tp'), may hold values from -0.15625 to 0.15625
- mix_taps: float32 [3, 768], P(None, 'tp'), may hold values from -3 to 3
- w_mix_out: bfloat16 [768, 1536], P('tp', 'fs'), may hold values from -0.625 to 0.625
- mix_post_gain: float32 [1536], replicated, may hold values from 0.1 to 1.9
- ffn_pre_gain: float32 [1536], replicated, may hold values from 0.1 to 1.9
- w_linear: bfloat16 [1536, 4224], P('fs', 'tp'), may hold values from -0.15625 to 0.15625
- w_gated: bfloat16 [1536, 4224], P('fs', 'tp'), may hold values from -0.15625 to 0.15625
- ffn_taps: float32 [3, 4224], P(None, 'tp'), may hold values from -3 to 3
- ffn_bias: float32 [4224], P('tp'), may hold values from -3 to 3
- w_down: bfloat16 [4224, 1536], P('tp', 'fs'), may hold values from -0.25 to 0.25
- ffn_post_gain: float32 [1536], replicated, may hold values from 0.1 to 1.9
Outputs:
- result: bfloat16 [32768, 1536], P(('rep', 'fs'))
The draws below stay inside these ranges and needn't reach their ends.
All inputs are finite; a program needn't handle non-finite values.
Results may differ from the reference program's by a relative error of at most 0.023.
Values may be sent and summed in bfloat16 or wider, within the bound.
No kernel may reach another device: no remote copies, remote signals or barrier semaphores. Data moves between devices by JAX's collectives and lax.ppermute only.
A program may use at most 64 MiB of HBM per device.

```python
import jax
import jax.numpy as jnp
from jax import lax

D = 1536
CONV_W = 768
FF = 4224
SEQ_LEN = 128
TOKENS = 32768
N_TP = 8


def spiked(entries, stream_key, source, target, blocks, factor):
    owner, partner = [(jnp.arange(entries.shape[position]) // (entries.shape[position] // blocks)).reshape([-1 if axis == position else 1 for axis in range(entries.ndim)]) for position in (source, target)]
    chosen = jax.random.permutation(stream_key, blocks)[partner]
    strong = (owner == chosen) | (owner == (partner + blocks // 2) % blocks)
    return jnp.where(strong, factor * entries, entries)


def block_levels(own_key, dims, shards, least, largest):
    factor_of, own = 1.0, jax.random.fold_in(own_key, 6)
    for axis_at, shards_of in shards:
        draws = jnp.exp(jax.random.uniform(jax.random.fold_in(own, axis_at), (shards_of,), jnp.float32, least / len(shards), largest / len(shards)))
        factor_of = factor_of * jnp.repeat(draws, dims[axis_at] // shards_of).reshape([-1 if axis == axis_at else 1 for axis in range(len(dims))])
    return factor_of


def scatter_about(stream_key, dims, deviation, limit, cuts=(), held_as=jnp.bfloat16):
    drawn = jax.random.normal(stream_key, dims, jnp.float32) * deviation
    if len(cuts) > 0:
        drawn = block_levels(stream_key, dims, cuts, -0.22, 0.18) * drawn
    return jnp.clip(drawn, min=-limit, max=limit).astype(held_as)


def gaussian_with(own_key, shape, scale, reach, shards, heavy, kind=jnp.bfloat16):
    values = scale * jax.random.normal(own_key, shape, jnp.float32)
    if shards:
        values = values * block_levels(own_key, shape, shards, -0.22, 0.18)
    return jnp.clip(spiked(values, jax.random.fold_in(own_key, 3), *heavy), -reach, reach).astype(kind)


def setup_inputs(seed: int = 0) -> dict:
    streams_of = jax.random.split(jax.random.key(seed), 16)
    stream = scatter_about(streams_of[0], (TOKENS, D), 1.0, 6.0, ((0, 128),))
    mix_pre_gain = jnp.clip(1.0 + 0.18 * jax.random.normal(streams_of[1], (D,), jnp.float32), 0.1, 1.9)
    w_outer_gate = scatter_about(streams_of[2], (D, CONV_W), D ** -0.5, 0.15625, ((0, 64), (1, 8)))
    w_inner_gate = scatter_about(streams_of[3], (D, CONV_W), D ** -0.5, 0.15625, ((0, 64), (1, 8)))
    w_value = scatter_about(streams_of[4], (D, CONV_W), D ** -0.5, 0.15625, ((0, 64), (1, 8)))
    mix_taps = scatter_about(streams_of[5], (3, CONV_W), 0.577, 3.0, ((1, 8),), jnp.float32)
    w_mix_out = gaussian_with(streams_of[6], (CONV_W, D), CONV_W ** -0.5, 0.625, ((0, 8), (1, 64)), (0, 1, 64, 4.0))
    mix_post_gain = jnp.clip(1.0 + 0.18 * jax.random.normal(streams_of[7], (D,), jnp.float32), 0.1, 1.9)
    ffn_pre_gain = jnp.clip(1.0 + 0.18 * jax.random.normal(streams_of[8], (D,), jnp.float32), 0.1, 1.9)
    w_linear = scatter_about(streams_of[9], (D, FF), D ** -0.5, 0.15625, ((0, 64), (1, 8)))
    w_gated = scatter_about(streams_of[10], (D, FF), D ** -0.5, 0.15625, ((0, 64), (1, 8)))
    ffn_taps = scatter_about(streams_of[11], (3, FF), 0.577, 3.0, ((1, 8),), jnp.float32)
    ffn_bias = scatter_about(streams_of[12], (FF,), 0.5, 3.0, ((0, 8),), jnp.float32)
    w_down = gaussian_with(streams_of[13], (FF, D), FF ** -0.5, 0.25, ((0, 8), (1, 64)), (0, 1, 64, 4.0))
    ffn_post_gain = jnp.clip(1.0 + 0.18 * jax.random.normal(streams_of[14], (D,), jnp.float32), 0.1, 1.9)
    return {"stream": stream, "mix_pre_gain": mix_pre_gain, "w_outer_gate": w_outer_gate, "w_inner_gate": w_inner_gate, "w_value": w_value, "mix_taps": mix_taps, "w_mix_out": w_mix_out, "mix_post_gain": mix_post_gain, "ffn_pre_gain": ffn_pre_gain, "w_linear": w_linear, "w_gated": w_gated, "ffn_taps": ffn_taps, "ffn_bias": ffn_bias, "w_down": w_down, "ffn_post_gain": ffn_post_gain}


EPS = 1e-06

def norm_scale(values, gain):
    return values * lax.rsqrt(lax.optimization_barrier(jnp.mean(values * values, axis=-1, keepdims=True)) + EPS) * gain

def conv_three(values, taps):
    height, breadth = values.shape
    grouped = values.reshape(height // SEQ_LEN, SEQ_LEN, breadth)
    padded = jnp.pad(grouped, ((0, 0), (1, 1), (0, 0)))
    mixed = taps[0] * padded[:, :-2] + taps[1] * padded[:, 1:-1] + taps[2] * padded[:, 2:]
    return mixed.reshape(height, breadth)

def blocked_sum(left, right):
    block_cols = left.shape[1] // N_TP
    summed = jnp.zeros((left.shape[0], right.shape[1]), jnp.float32)
    for block in range(N_TP):
        partial_value = jnp.dot(left[:, block * block_cols:(block + 1) * block_cols], right[block * block_cols:(block + 1) * block_cols], preferred_element_type=jnp.float32)
        rounded = lax.optimization_barrier(partial_value.astype(jnp.bfloat16))
        summed = summed + rounded.astype(jnp.float32)
    return summed.astype(jnp.bfloat16)

def reference(stream, mix_pre_gain, w_outer_gate, w_inner_gate, w_value, mix_taps, w_mix_out, mix_post_gain, ffn_pre_gain, w_linear, w_gated, ffn_taps, ffn_bias, w_down, ffn_post_gain):
    resid = stream.astype(jnp.float32)
    normed = norm_scale(resid, mix_pre_gain).astype(jnp.bfloat16)
    outer = jnp.dot(normed, w_outer_gate, preferred_element_type=jnp.float32).astype(jnp.bfloat16)
    inner = jnp.dot(normed, w_inner_gate, preferred_element_type=jnp.float32).astype(jnp.bfloat16)
    value = jnp.dot(normed, w_value, preferred_element_type=jnp.float32).astype(jnp.bfloat16)
    product = inner.astype(jnp.float32) * value.astype(jnp.float32)
    mixed = (outer.astype(jnp.float32) * conv_three(product, mix_taps)).astype(jnp.bfloat16)
    branch = blocked_sum(mixed, w_mix_out)
    middle = (resid + norm_scale(branch.astype(jnp.float32), mix_post_gain)).astype(jnp.bfloat16)
    middle_f = middle.astype(jnp.float32)
    normed_two = norm_scale(middle_f, ffn_pre_gain).astype(jnp.bfloat16)
    linear = jnp.dot(normed_two, w_linear, preferred_element_type=jnp.float32).astype(jnp.bfloat16)
    gated = jnp.dot(normed_two, w_gated, preferred_element_type=jnp.float32).astype(jnp.bfloat16)
    activated = jax.nn.gelu(conv_three(gated.astype(jnp.float32), ffn_taps) + ffn_bias, approximate=True)
    hidden = (activated * linear.astype(jnp.float32)).astype(jnp.bfloat16)
    branch_two = blocked_sum(hidden, w_down)
    return (middle_f + norm_scale(branch_two.astype(jnp.float32), ffn_post_gain)).astype(jnp.bfloat16)
```

```python
import jax
import jax.numpy as jnp
from jax import lax
from jax.sharding import Mesh
from jax.sharding import PartitionSpec as P

SEQ_LEN = 128
FS = ("fs_0", "fs_1")
REP_FS = ("rep", "fs_0", "fs_1")
EPS = 1e-06
F32 = jnp.float32
BF16 = jnp.bfloat16


def of_reps(first, second):
    return jnp.where(lax.axis_index("rep") == 0, first, second)


def plane_gathered(first, second):
    mine = of_reps(first, second)
    both = lax.all_gather(mine, REP_FS, axis=0, tiled=True)
    rows = both.shape[0] // 2
    return both[:rows], both[rows:]


def norm_scale(values, gain):
    return values * lax.rsqrt(jnp.mean(values * values, axis=-1, keepdims=True) + EPS) * gain


def conv_three(values, taps):
    height, breadth = values.shape
    grouped = values.reshape(height // SEQ_LEN, SEQ_LEN, breadth)
    padded = jnp.pad(grouped, ((0, 0), (1, 1), (0, 0)))
    mixed = taps[0] * padded[:, :-2] + taps[1] * padded[:, 1:-1] + taps[2] * padded[:, 2:]
    return mixed.reshape(height, breadth)


def dot(a, b):
    return jnp.dot(a, b, preferred_element_type=F32)


def dot_t(a, b):
    return lax.dot_general(a, b, (((1,), (1,)), ((), ())), preferred_element_type=F32)


def rows_summed(partial_value):
    n = lax.axis_size("tp")
    tiles = partial_value.astype(BF16).reshape(n, -1, partial_value.shape[1])
    arrived = lax.all_to_all(tiles, "tp", split_axis=0, concat_axis=0, tiled=True)
    return arrived.astype(F32).sum(axis=0).astype(BF16).astype(F32)


def rows_gathered(x):
    n = lax.axis_size("tp")
    tiles = lax.all_to_all(jnp.broadcast_to(x[None], (n, *x.shape)), "tp", 0, 0, tiled=True)
    return tiles.reshape(-1, x.shape[1])


def on_device(
    stream,
    mix_pre_gain,
    w_outer_gate,
    w_inner_gate,
    w_value,
    mix_taps,
    w_mix_out,
    mix_post_gain,
    ffn_pre_gain,
    w_linear,
    w_gated,
    ffn_taps,
    ffn_bias,
    w_down,
    ffn_post_gain,
):
    width = w_value.shape[1]
    hidden_w = w_linear.shape[1]
    split = hidden_w // 256 * 128
    tail = hidden_w - 2 * split
    down_t = w_down.T
    first_mix, second_mix = plane_gathered(
        jnp.concatenate([w_outer_gate, w_inner_gate], axis=1),
        jnp.concatenate([w_value, w_mix_out.T], axis=1),
    )
    down_tail = down_t[:, 2 * split :]
    first_up, second_up = plane_gathered(
        jnp.concatenate([w_linear, down_tail], axis=1),
        jnp.concatenate([w_gated, down_tail], axis=1),
    )
    first_down, second_down = plane_gathered(down_t[:, :split], down_t[:, split : 2 * split])

    resid = stream.astype(F32)
    normed = norm_scale(resid, mix_pre_gain).astype(BF16)
    outer_inner = dot(normed, first_mix).astype(BF16).astype(F32)
    outer, inner = outer_inner[:, :width], outer_inner[:, width:]
    value = dot(normed, second_mix[:, :width]).astype(BF16).astype(F32)
    mixed = (outer * conv_three(inner * value, mix_taps)).astype(BF16)
    branch = rows_summed(dot_t(mixed, second_mix[:, width:]))
    rows = branch.shape[0]
    own = lax.dynamic_slice_in_dim(stream, lax.axis_index("tp") * rows, rows, 0).astype(F32)
    middle = (own + norm_scale(branch, mix_post_gain)).astype(BF16).astype(F32)
    normed_two = rows_gathered(norm_scale(middle, ffn_pre_gain).astype(BF16))

    linear = dot(normed_two, first_up[:, :hidden_w]).astype(BF16).astype(F32)
    gated = dot(normed_two, second_up[:, :hidden_w]).astype(BF16).astype(F32)
    activated = jax.nn.gelu(conv_three(gated, ffn_taps) + ffn_bias, approximate=True)
    hidden = (activated * linear).astype(BF16)
    partial_two = dot_t(hidden[:, :split], first_down)
    partial_two += dot_t(hidden[:, split : 2 * split], second_down)
    partial_two += dot_t(hidden[:, 2 * split :], first_up[:, hidden_w : hidden_w + tail])
    branch_two = rows_summed(partial_two)
    return rows_gathered((middle + norm_scale(branch_two, ffn_post_gain)).astype(BF16))


def solution(mesh):
    split = Mesh(
        mesh.devices.reshape(mesh.shape["rep"], 8, 8, mesh.shape["tp"]),
        ("rep", "fs_0", "fs_1", "tp"),
    )
    return jax.shard_map(
        on_device,
        mesh=split,
        in_specs=(
            P(REP_FS, None),
            P(),
            P(FS, "tp"),
            P(FS, "tp"),
            P(FS, "tp"),
            P(None, "tp"),
            P("tp", FS),
            P(),
            P(),
            P(FS, "tp"),
            P(FS, "tp"),
            P(None, "tp"),
            P("tp"),
            P("tp", FS),
            P(),
        ),
        out_specs=P(REP_FS, None),
        check_vma=False,
    )
```

```python
import jax
import jax.numpy as jnp
from jax import lax
from jax.sharding import Mesh
from jax.sharding import PartitionSpec as P

SEQ_LEN = 128
FS = ("fs_0", "fs_1")
REP_FS = ("rep", "fs_0", "fs_1")
EPS = 1e-06
F32 = jnp.float32
BF16 = jnp.bfloat16
LANES = 128


def from_ahead(x, steps):
    n = lax.axis_size("rep") * lax.axis_size("fs_0")
    return lax.ppermute(x, ("rep", "fs_0"), [(i, (i - steps) % n) for i in range(n)])


def doubled(x, sign):
    n = lax.axis_size("fs_0")
    rows = x.shape[0]
    offsets, step = [0], n // 2
    while step:
        x = jnp.concatenate([x, from_ahead(x, sign * step)], axis=0)
        offsets += [o + sign * step for o in offsets]
        step //= 2
    where = [o % n for o in offsets]
    order = [where.index(k) for k in range(n)]
    return [x[k * rows : (k + 1) * rows] for k in order]


def norm_scale(values, gain):
    return values * lax.rsqrt(jnp.mean(values * values, axis=-1, keepdims=True) + EPS) * gain


def conv_three(values, taps):
    height, breadth = values.shape
    grouped = values.reshape(height // SEQ_LEN, SEQ_LEN, breadth)
    padded = jnp.pad(grouped, ((0, 0), (1, 1), (0, 0)))
    mixed = taps[0] * padded[:, :-2] + taps[1] * padded[:, 1:-1] + taps[2] * padded[:, 2:]
    return mixed.reshape(height, breadth)


def dot(a, b):
    return jnp.dot(a, b, preferred_element_type=F32)


def dot_t(a, b):
    return lax.dot_general(a, b, (((1,), (1,)), ((), ())), preferred_element_type=F32)


def sent_to_all(x, axis):
    n = lax.axis_size(axis)
    tiles = lax.all_to_all(jnp.broadcast_to(x[None], (n, *x.shape)), axis, 0, 0, tiled=True)
    return tiles.reshape(-1, x.shape[1])


def rows_summed(partial_value):
    n = lax.axis_size("tp")
    tiles = partial_value.astype(BF16).reshape(n, -1, partial_value.shape[1])
    arrived = lax.all_to_all(tiles, "tp", split_axis=0, concat_axis=0, tiled=True)
    return arrived.astype(F32).sum(axis=0).astype(BF16).astype(F32)


def on_device(
    stream,
    mix_pre_gain,
    w_outer_gate,
    w_inner_gate,
    w_value,
    mix_taps,
    w_mix_out,
    mix_post_gain,
    ffn_pre_gain,
    w_linear,
    w_gated,
    ffn_taps,
    ffn_bias,
    w_down,
    ffn_post_gain,
):
    width = w_value.shape[1]
    hidden_w = w_linear.shape[1]
    rows = w_value.shape[0]
    n0, n1 = lax.axis_size("fs_0"), lax.axis_size("fs_1")
    d = stream.shape[1]

    mix_cols = jnp.concatenate([w_outer_gate, w_inner_gate, w_value, w_mix_out.T], axis=1)
    ffn_cols = jnp.concatenate([w_linear, w_gated, w_down.T], axis=1)
    cut = max(0, ((mix_cols.shape[1] + ffn_cols.shape[1]) // 2 - mix_cols.shape[1]) // LANES + 1) * LANES
    one_way = doubled(jnp.concatenate([mix_cols, ffn_cols[:, :cut]], axis=1), 1)
    other_way = doubled(ffn_cols[:, cut:], -1)
    mix_part = jnp.concatenate([b[:, : mix_cols.shape[1]] for b in one_way], axis=0)
    ffn_part = jnp.concatenate(
        [
            jnp.concatenate([b[:, mix_cols.shape[1] :] for b in one_way], axis=0),
            jnp.concatenate(other_way, axis=0),
        ],
        axis=1,
    )
    ffn_full = lax.all_gather(ffn_part, "fs_1", axis=0, tiled=True)
    mix_in = lax.all_gather(mix_part[:, : 3 * width], "fs_1", axis=0, tiled=True)
    mix_out = sent_to_all(mix_part[:, 3 * width :], "fs_1")

    place = jnp.arange(d)
    ahead = place // rows % n0
    z = (lax.axis_index("fs_0") + ahead) % n0
    source = z * (n1 * rows) + place // (rows * n0) * rows + place % rows
    chosen = (jnp.arange(d)[:, None] == source[None, :]).astype(BF16)

    def turned(gain):
        blocks = gain.reshape(n0, n1, rows)
        twice = jnp.concatenate([blocks, blocks], axis=0)
        mine = lax.dynamic_slice_in_dim(twice, lax.axis_index("fs_0"), n0, 0)
        return mine.transpose(1, 0, 2).reshape(-1)

    stream = dot(stream, chosen).astype(BF16)
    resid = stream.astype(F32)
    normed = norm_scale(resid, turned(mix_pre_gain)).astype(BF16)
    three = dot(normed, mix_in).astype(BF16).astype(F32)
    outer, inner, value = three[:, :width], three[:, width : 2 * width], three[:, 2 * width :]
    mixed = (outer * conv_three(inner * value, mix_taps)).astype(BF16)
    branch = rows_summed(dot_t(mixed, mix_out))
    own_rows = branch.shape[0]
    own = lax.dynamic_slice_in_dim(stream, lax.axis_index("tp") * own_rows, own_rows, 0)
    middle = own.astype(F32) + norm_scale(branch, turned(mix_post_gain))
    middle = middle.astype(BF16).astype(F32)
    normed_two = sent_to_all(norm_scale(middle, turned(ffn_pre_gain)).astype(BF16), "tp")

    both = dot(normed_two, ffn_full[:, : 2 * hidden_w]).astype(BF16).astype(F32)
    linear, gated = both[:, :hidden_w], both[:, hidden_w:]
    activated = jax.nn.gelu(conv_three(gated, ffn_taps) + ffn_bias, approximate=True)
    hidden = (activated * linear).astype(BF16)
    branch_two = rows_summed(dot_t(hidden, ffn_full[:, 2 * hidden_w :]))
    result = (middle + norm_scale(branch_two, turned(ffn_post_gain))).astype(BF16)
    return sent_to_all(dot_t(result, chosen).astype(BF16), "tp")


def solution(mesh):
    tp = mesh.shape["tp"]
    split = Mesh(mesh.devices.reshape(mesh.shape["rep"], 8, 8, tp), ("rep", "fs_0", "fs_1", "tp"))
    return jax.shard_map(
        on_device,
        mesh=split,
        in_specs=(
            P(REP_FS, None),
            P(),
            P(FS, "tp"),
            P(FS, "tp"),
            P(FS, "tp"),
            P(None, "tp"),
            P("tp", FS),
            P(),
            P(),
            P(FS, "tp"),
            P(FS, "tp"),
            P(None, "tp"),
            P("tp"),
            P("tp", FS),
            P(),
        ),
        out_specs=P(REP_FS, None),
        check_vma=False,
    )
```

```python
import jax
import jax.numpy as jnp
from jax import lax
from jax.sharding import Mesh
from jax.sharding import PartitionSpec as P

SEQ_LEN = 128
FS = ("fs_0", "fs_1")
TP = ("x", "core")
REP_FS = ("rep", "fs_0", "fs_1")
EPS = 1e-06
F32 = jnp.float32
BF16 = jnp.bfloat16


def from_ahead(x, steps):
    n = lax.axis_size("rep") * lax.axis_size("fs_0")
    return lax.ppermute(x, ("rep", "fs_0"), [(i, (i - steps) % n) for i in range(n)])


def doubled(x, sign):
    n = lax.axis_size("fs_0")
    offsets, step = [0], n // 2
    while step:
        arrived = from_ahead(x, sign * step)
        x = jnp.concatenate([x, arrived], axis=0)
        offsets += [o + sign * step for o in offsets]
        step //= 2
    return x, [o % n for o in offsets]


def other_core(x):
    return lax.ppermute(x, "core", [(0, 1), (1, 0)])


def norm_scale(values, gain):
    return values * lax.rsqrt(jnp.mean(values * values, axis=-1, keepdims=True) + EPS) * gain


def conv_three(values, taps):
    height, breadth = values.shape
    grouped = values.reshape(height // SEQ_LEN, SEQ_LEN, breadth)
    padded = jnp.pad(grouped, ((0, 0), (1, 1), (0, 0)))
    mixed = taps[0] * padded[:, :-2] + taps[1] * padded[:, 1:-1] + taps[2] * padded[:, 2:]
    return mixed.reshape(height, breadth)


def dot(a, b):
    return jnp.dot(a, b, preferred_element_type=F32)


def dot_t(a, b):
    return lax.dot_general(a, b, (((1,), (1,)), ((), ())), preferred_element_type=F32)


def sent_to_all(x, axis):
    n = lax.axis_size(axis)
    tiles = lax.all_to_all(jnp.broadcast_to(x[None], (n, *x.shape)), axis, 0, 0, tiled=True)
    return tiles.reshape(-1, x.shape[1])


def rows_summed(partial_value):
    n = lax.axis_size("x")
    tiles = partial_value.astype(BF16).reshape(n, -1, partial_value.shape[1])
    arrived = lax.all_to_all(tiles, "x", split_axis=0, concat_axis=0, tiled=True)
    return arrived.astype(F32).sum(axis=0).astype(BF16).astype(F32)


def layer(
    stream,
    mix_pre_gain,
    w_outer_gate,
    w_inner_gate,
    w_value,
    mix_taps,
    w_mix_out,
    mix_post_gain,
    ffn_pre_gain,
    w_linear,
    w_gated,
    ffn_taps,
    ffn_bias,
    w_down,
    ffn_post_gain,
):
    width = w_value.shape[1]
    hidden_w = w_linear.shape[1]
    rows = w_value.shape[0]
    n0, n1 = lax.axis_size("fs_0"), lax.axis_size("fs_1")
    d = stream.shape[1]
    core = lax.axis_index("core")

    ffn_cols = jnp.concatenate([w_linear, w_gated, w_down.T], axis=1)
    ffn_part, offsets = doubled(ffn_cols, 1)
    ffn_full = lax.all_gather(ffn_part, ("core", "fs_1"), axis=0, tiled=True)
    ffn_full = [ffn_full[:d], ffn_full[d:]]

    mix_cols = jnp.concatenate([w_outer_gate, w_inner_gate, w_value, w_mix_out.T], axis=1)
    mix_part = sent_to_all(mix_cols, "fs_1")
    mix_part, back = doubled(mix_part, -1)
    mix_part = mix_part.reshape(n0, n1, rows, mix_cols.shape[1])
    mix_own = jnp.stack([mix_part[back.index(o)] for o in offsets], axis=1).reshape(d, -1)
    mix_full = [mix_own, other_core(mix_own)]

    small = jnp.concatenate(
        [ffn_taps, ffn_bias[None], jnp.pad(mix_taps, ((0, 0), (0, hidden_w - width)))], axis=0
    )
    small = [small, other_core(small)]
    mix_taps = [s[4:7, :width] for s in small]
    small = [jnp.where(core == 0, small[0], small[1]), jnp.where(core == 0, small[1], small[0])]

    place = jnp.arange(d)
    k = place // rows % n0
    ahead = sum(jnp.where(k == i, o, 0) for i, o in enumerate(offsets))
    z = (lax.axis_index("fs_0") + ahead) % n0
    source = z * (n1 * rows) + place // (rows * n0) * rows + place % rows
    chosen = (jnp.arange(d)[:, None] == source[None, :]).astype(BF16)

    def turned(gain):
        blocks = gain.reshape(n0, n1, rows)
        twice = jnp.concatenate([blocks, blocks], axis=0)
        mine = lax.dynamic_slice_in_dim(twice, lax.axis_index("fs_0"), n0, 0)
        return jnp.stack([mine[o] for o in offsets], axis=1).reshape(-1)

    half = stream.shape[0] // 2
    stream = lax.dynamic_slice_in_dim(stream, core * half, half, 0)
    stream = dot(stream, chosen).astype(BF16)
    resid = stream.astype(F32)
    normed = norm_scale(resid, turned(mix_pre_gain)).astype(BF16)
    partial_value = 0.0
    for weights, taps in zip(mix_full, mix_taps):
        three = dot(normed, weights[:, : 3 * width]).astype(BF16).astype(F32)
        outer, inner, value = jnp.split(three, 3, axis=1)
        mixed = (outer * conv_three(inner * value, taps)).astype(BF16)
        partial_value = partial_value + dot_t(mixed, weights[:, 3 * width :])
    branch = rows_summed(partial_value)
    own_rows = branch.shape[0]
    own = lax.dynamic_slice_in_dim(stream, lax.axis_index("x") * own_rows, own_rows, 0)
    middle = own.astype(F32) + norm_scale(branch, turned(mix_post_gain))
    middle = middle.astype(BF16).astype(F32)
    normed_two = sent_to_all(norm_scale(middle, turned(ffn_pre_gain)).astype(BF16), "x")

    partial_two = 0.0
    for weights, extra in zip(ffn_full, small):
        both = dot(normed_two, weights[:, : 2 * hidden_w]).astype(BF16).astype(F32)
        linear, gated = both[:, :hidden_w], both[:, hidden_w:]
        activated = jax.nn.gelu(conv_three(gated, extra[:3]) + extra[3], approximate=True)
        hidden = (activated * linear).astype(BF16)
        partial_two = partial_two + dot_t(hidden, weights[:, 2 * hidden_w :])
    branch_two = rows_summed(partial_two)
    result = (middle + norm_scale(branch_two, turned(ffn_post_gain))).astype(BF16)
    result = sent_to_all(dot_t(result, chosen).astype(BF16), "x")
    return lax.all_gather(result, "core", axis=0, tiled=True)


def solution(mesh):
    split = Mesh(
        mesh.devices.reshape(mesh.shape["rep"], 8, 8, mesh.shape["tp"] // 2, 2),
        ("rep", "fs_0", "fs_1", "x", "core"),
    )
    return jax.shard_map(
        layer,
        mesh=split,
        in_specs=(
            P(REP_FS, None),
            P(),
            P(FS, TP),
            P(FS, TP),
            P(FS, TP),
            P(None, TP),
            P(TP, FS),
            P(),
            P(),
            P(FS, TP),
            P(FS, TP),
            P(None, TP),
            P(TP),
            P(TP, FS),
            P(),
        ),
        out_specs=P(REP_FS, None),
        check_vma=False,
    )
```

```python
import jax
import jax.numpy as jnp
from jax import lax
from jax.sharding import Mesh
from jax.sharding import PartitionSpec as P

SEQ_LEN = 128
FS = ("fs_0", "fs_1")
TP = ("x", "core")
REP_FS = ("rep", "fs_0", "fs_1")
EPS = 1e-06
F32 = jnp.float32
BF16 = jnp.bfloat16


def from_ahead(x, steps):
    n = lax.axis_size("rep") * lax.axis_size("fs_0")
    return lax.ppermute(x, ("rep", "fs_0"), [(i, (i - steps) % n) for i in range(n)])


def doubled(x, offsets, steps, sign):
    for step in steps:
        arrived = from_ahead(x, sign * step)
        x = jnp.concatenate([x, arrived], axis=0)
        offsets = offsets + [o + sign * step for o in offsets]
    return x, [o % lax.axis_size("fs_0") for o in offsets]


def other_core(x):
    return lax.ppermute(x, "core", [(0, 1), (1, 0)])


def norm_scale(values, gain):
    return values * lax.rsqrt(jnp.mean(values * values, axis=-1, keepdims=True) + EPS) * gain


def conv_three(values, taps):
    height, breadth = values.shape
    grouped = values.reshape(height // SEQ_LEN, SEQ_LEN, breadth)
    padded = jnp.pad(grouped, ((0, 0), (1, 1), (0, 0)))
    mixed = taps[0] * padded[:, :-2] + taps[1] * padded[:, 1:-1] + taps[2] * padded[:, 2:]
    return mixed.reshape(height, breadth)


def dot(a, b):
    return jnp.dot(a, b, preferred_element_type=F32)


def dot_t(a, b):
    return lax.dot_general(a, b, (((1,), (1,)), ((), ())), preferred_element_type=F32)


def sent_to_all(x, axis):
    n = lax.axis_size(axis)
    tiles = lax.all_to_all(jnp.broadcast_to(x[None], (n, *x.shape)), axis, 0, 0, tiled=True)
    return tiles.reshape(-1, x.shape[1])


def rows_summed(partial_value):
    n = lax.axis_size("x")
    tiles = partial_value.astype(BF16).reshape(n, -1, partial_value.shape[1])
    arrived = lax.all_to_all(tiles, "x", split_axis=0, concat_axis=0, tiled=True)
    return arrived.astype(F32).sum(axis=0).astype(BF16).astype(F32)


def layer(
    stream,
    mix_pre_gain,
    w_outer_gate,
    w_inner_gate,
    w_value,
    mix_taps,
    w_mix_out,
    mix_post_gain,
    ffn_pre_gain,
    w_linear,
    w_gated,
    ffn_taps,
    ffn_bias,
    w_down,
    ffn_post_gain,
):
    width = w_value.shape[1]
    hidden_w = w_linear.shape[1]
    rows = w_value.shape[0]
    n0, n1 = lax.axis_size("fs_0"), lax.axis_size("fs_1")
    d = stream.shape[1]
    core = lax.axis_index("core")

    ffn_cols = jnp.concatenate([w_linear, w_gated, w_down.T], axis=1)
    ffn_part, offsets = doubled(ffn_cols, [0], (4, 2, 1), 1)
    ffn_full = lax.all_gather(ffn_part, ("core", "fs_1"), axis=0, tiled=True)
    ffn_full = [ffn_full[:d], ffn_full[d:]]

    mix_cols = jnp.concatenate([w_outer_gate, w_inner_gate, w_value, w_mix_out.T], axis=1)
    mix_part = sent_to_all(mix_cols, "fs_1")
    mix_part, near = doubled(mix_part, [0], (4,), -1)
    mix_part = mix_part.reshape(len(near), 2, -1, mix_part.shape[1])
    ways = []
    for way, sign in ((0, -1), (1, 1)):
        mine = mix_part[:, way].reshape(-1, mix_part.shape[3])
        mine, back = doubled(mine, near, (2, 1), sign)
        mine = mine.reshape(n0, n1 // 2, rows, -1)
        ways.append(jnp.stack([mine[back.index(o)] for o in offsets], axis=1))
    mix_own = jnp.concatenate(ways, axis=0).reshape(d, -1)
    mix_full = [mix_own, other_core(mix_own)]

    small = jnp.concatenate(
        [ffn_taps, ffn_bias[None], jnp.pad(mix_taps, ((0, 0), (0, hidden_w - width)))], axis=0
    )
    small = [small, other_core(small)]
    mix_taps = [s[4:7, :width] for s in small]
    small = [jnp.where(core == 0, small[0], small[1]), jnp.where(core == 0, small[1], small[0])]

    place = jnp.arange(d)
    k = place // rows % n0
    ahead = sum(jnp.where(k == i, o, 0) for i, o in enumerate(offsets))
    z = (lax.axis_index("fs_0") + ahead) % n0
    source = z * (n1 * rows) + place // (rows * n0) * rows + place % rows
    chosen = (jnp.arange(d)[:, None] == source[None, :]).astype(BF16)

    def turned(gain):
        blocks = gain.reshape(n0, n1, rows)
        twice = jnp.concatenate([blocks, blocks], axis=0)
        mine = lax.dynamic_slice_in_dim(twice, lax.axis_index("fs_0"), n0, 0)
        return jnp.stack([mine[o] for o in offsets], axis=1).reshape(-1)

    half = stream.shape[0] // 2
    stream = lax.dynamic_slice_in_dim(stream, core * half, half, 0)
    stream = dot(stream, chosen).astype(BF16)
    resid = stream.astype(F32)
    normed = norm_scale(resid, turned(mix_pre_gain)).astype(BF16)
    partial_value = 0.0
    for weights, taps in zip(mix_full, mix_taps):
        three = dot(normed, weights[:, : 3 * width]).astype(BF16).astype(F32)
        outer, inner, value = jnp.split(three, 3, axis=1)
        mixed = (outer * conv_three(inner * value, taps)).astype(BF16)
        partial_value = partial_value + dot_t(mixed, weights[:, 3 * width :])
    branch = rows_summed(partial_value)
    own_rows = branch.shape[0]
    own = lax.dynamic_slice_in_dim(stream, lax.axis_index("x") * own_rows, own_rows, 0)
    middle = own.astype(F32) + norm_scale(branch, turned(mix_post_gain))
    middle = middle.astype(BF16).astype(F32)
    normed_two = sent_to_all(norm_scale(middle, turned(ffn_pre_gain)).astype(BF16), "x")

    partial_two = 0.0
    for weights, extra in zip(ffn_full, small):
        both = dot(normed_two, weights[:, : 2 * hidden_w]).astype(BF16).astype(F32)
        linear, gated = both[:, :hidden_w], both[:, hidden_w:]
        activated = jax.nn.gelu(conv_three(gated, extra[:3]) + extra[3], approximate=True)
        hidden = (activated * linear).astype(BF16)
        partial_two = partial_two + dot_t(hidden, weights[:, 2 * hidden_w :])
    branch_two = rows_summed(partial_two)
    result = (middle + norm_scale(branch_two, turned(ffn_post_gain))).astype(BF16)
    result = sent_to_all(dot_t(result, chosen).astype(BF16), "x")
    return lax.all_gather(result, "core", axis=0, tiled=True)


def solution(mesh):
    split = Mesh(
        mesh.devices.reshape(mesh.shape["rep"], 8, 8, mesh.shape["tp"] // 2, 2),
        ("rep", "fs_0", "fs_1", "x", "core"),
    )
    return jax.shard_map(
        layer,
        mesh=split,
        in_specs=(
            P(REP_FS, None),
            P(),
            P(FS, TP),
            P(FS, TP),
            P(FS, TP),
            P(None, TP),
            P(TP, FS),
            P(),
            P(),
            P(FS, TP),
            P(FS, TP),
            P(None, TP),
            P(TP),
            P(TP, FS),
            P(),
        ),
        out_specs=P(REP_FS, None),
        check_vma=False,
    )
```

```python
import jax
import jax.numpy as jnp
from jax import lax
from jax.experimental import pallas as pl
from jax.experimental.pallas import tpu as pltpu
from jax.sharding import Mesh
from jax.sharding import PartitionSpec as P

SEQ_LEN = 128
FS = ("fs_0", "fs_1")
TP = ("x", "core")
REP_FS = ("rep", "fs_0", "fs_1")
EPS = 1e-06
F32 = jnp.float32
BF16 = jnp.bfloat16
LANES = 128
BLOCK_ROWS = 512


def from_ahead(x, steps):
    n = lax.axis_size("rep") * lax.axis_size("fs_0")
    return lax.ppermute(x, ("rep", "fs_0"), [(i, (i - steps) % n) for i in range(n)])


def doubled(x, offsets, steps, sign):
    for step in steps:
        arrived = from_ahead(x, sign * step)
        x = jnp.concatenate([x, arrived], axis=0)
        offsets = offsets + [o + sign * step for o in offsets]
    return x, [o % lax.axis_size("fs_0") for o in offsets]


def other_core(x):
    return lax.ppermute(x, "core", [(0, 1), (1, 0)])


def ffn_kernel(x_ref, extra_ref, weights_ref, out_ref, held, arrived, *, main, tail):
    tokens, d = x_ref.shape
    blocks = d // BLOCK_ROWS
    copies = []
    for i in range(2 * blocks):
        rows = pl.ds(i * BLOCK_ROWS, BLOCK_ROWS)
        copies.append(pltpu.make_async_copy(weights_ref.at[rows], held.at[rows], arrived.at[i]))
        copies[-1].start()
    row = lax.broadcasted_iota(jnp.int32, (tokens, LANES), 0)
    lane = lax.broadcasted_iota(jnp.int32, (tokens, LANES), 1)

    def hidden_of(linear, gated, extra):
        linear, gated = linear.astype(BF16).astype(F32), gated.astype(BF16).astype(F32)
        before = jnp.where(row == 0, 0.0, pltpu.roll(gated, 1, 0))
        after = jnp.where(row == tokens - 1, 0.0, pltpu.roll(gated, tokens - 1, 0))
        mixed = extra[0:1] * before + extra[1:2] * gated + extra[2:3] * after + extra[3:4]
        return jax.nn.gelu(mixed, approximate=True) * linear

    total = jnp.zeros((tokens, d), F32)
    for core in range(2):
        up = jnp.zeros((tokens, 2 * main), F32)
        tails = jnp.zeros((tokens, LANES), F32)
        for k in range(blocks):
            copies[core * blocks + k].wait()
            x = x_ref[:, k * BLOCK_ROWS : (k + 1) * BLOCK_ROWS]
            rows = pl.ds((core * blocks + k) * BLOCK_ROWS, BLOCK_ROWS)
            up += jnp.dot(x, held[rows, : 2 * main], preferred_element_type=F32)
            tails += jnp.dot(x, held[rows, 3 * main :], preferred_element_type=F32)
        rows = pl.ds(core * d, d)
        for at in range(0, main, 2 * LANES):
            parts = []
            for j in range(at, at + 2 * LANES, LANES):
                extra = extra_ref[core, :, j : j + LANES]
                parts.append(
                    hidden_of(up[:, j : j + LANES], up[:, main + j : main + j + LANES], extra)
                )
            hidden = jnp.concatenate(parts, axis=1).astype(BF16)
            total += lax.dot_general(
                hidden,
                held[rows, 2 * main + at : 2 * main + at + 2 * LANES],
                (((1,), (1,)), ((), ())),
                preferred_element_type=F32,
            )
        gated = pltpu.roll(tails, LANES - tail, 1)
        hidden = hidden_of(tails, gated, extra_ref[core, :, main : main + LANES])
        hidden = pltpu.roll(jnp.where(lane < tail, hidden, 0.0), 2 * tail, 1).astype(BF16)
        total += lax.dot_general(
            hidden, held[rows, 3 * main :], (((1,), (1,)), ((), ())), preferred_element_type=F32
        )
    out_ref[...] = total.astype(BF16)


def ffn(x, extra, weights, main, tail):
    tokens, d = x.shape
    return pl.pallas_call(
        lambda *refs: ffn_kernel(*refs, main=main, tail=tail),
        out_shape=jax.ShapeDtypeStruct((tokens, d), BF16),
        in_specs=[
            pl.BlockSpec(memory_space=pltpu.VMEM),
            pl.BlockSpec(memory_space=pltpu.VMEM),
            pl.BlockSpec(memory_space=pltpu.HBM),
        ],
        out_specs=pl.BlockSpec(memory_space=pltpu.VMEM),
        scratch_shapes=[
            pltpu.VMEM(weights.shape, BF16),
            pltpu.SemaphoreType.DMA((2 * d // BLOCK_ROWS,)),
        ],
        compiler_params=pltpu.CompilerParams(vmem_limit_bytes=55 * 1024 * 1024),
        cost_estimate=pl.CostEstimate(
            flops=2 * tokens * weights.size, bytes_accessed=2 * weights.size, transcendentals=0
        ),
        name="ffn",
    )(x, extra, weights)


def norm_scale(values, gain):
    return values * lax.rsqrt(jnp.mean(values * values, axis=-1, keepdims=True) + EPS) * gain


def conv_three(values, taps):
    height, breadth = values.shape
    grouped = values.reshape(height // SEQ_LEN, SEQ_LEN, breadth)
    padded = jnp.pad(grouped, ((0, 0), (1, 1), (0, 0)))
    mixed = taps[0] * padded[:, :-2] + taps[1] * padded[:, 1:-1] + taps[2] * padded[:, 2:]
    return mixed.reshape(height, breadth)


def dot(a, b):
    return jnp.dot(a, b, preferred_element_type=F32)


def dot_t(a, b):
    return lax.dot_general(a, b, (((1,), (1,)), ((), ())), preferred_element_type=F32)


def sent_to_all(x, axis):
    n = lax.axis_size(axis)
    tiles = lax.all_to_all(jnp.broadcast_to(x[None], (n, *x.shape)), axis, 0, 0, tiled=True)
    return tiles.reshape(-1, x.shape[1])


def rows_summed(partial_value):
    n = lax.axis_size("x")
    tiles = partial_value.astype(BF16).reshape(n, -1, partial_value.shape[1])
    arrived = lax.all_to_all(tiles, "x", split_axis=0, concat_axis=0, tiled=True)
    return arrived.astype(F32).sum(axis=0).astype(BF16).astype(F32)


def layer(
    stream,
    mix_pre_gain,
    w_outer_gate,
    w_inner_gate,
    w_value,
    mix_taps,
    w_mix_out,
    mix_post_gain,
    ffn_pre_gain,
    w_linear,
    w_gated,
    ffn_taps,
    ffn_bias,
    w_down,
    ffn_post_gain,
):
    width = w_value.shape[1]
    hidden_w = w_linear.shape[1]
    rows = w_value.shape[0]
    n0, n1 = lax.axis_size("fs_0"), lax.axis_size("fs_1")
    d = stream.shape[1]
    core = lax.axis_index("core")

    main = hidden_w // (2 * LANES) * (2 * LANES)
    tail = hidden_w - main
    pieces = [w_linear, w_gated, w_down.T]
    spare = jnp.zeros((rows, LANES - 3 * tail), BF16)
    ffn_cols = jnp.concatenate(
        [p[:, :main] for p in pieces] + [p[:, main:] for p in pieces] + [spare], axis=1
    )
    ffn_part, offsets = doubled(ffn_cols, [0], (4,), 1)
    cut = ffn_cols.shape[1] // (2 * LANES) * LANES
    left = from_ahead(ffn_part[:, :cut], 2)
    right = from_ahead(ffn_part[:, cut:], -2)
    right = jnp.concatenate([right[rows:], right[:rows]], axis=0)
    ffn_part = jnp.concatenate([ffn_part, jnp.concatenate([left, right], axis=1)], axis=0)
    ffn_part, offsets = doubled(ffn_part, offsets + [2, 6], (1,), 1)
    ffn_full = lax.all_gather(ffn_part, ("core", "fs_1"), axis=0, tiled=True)

    mix_cols = jnp.concatenate([w_outer_gate, w_inner_gate, w_value, w_mix_out.T], axis=1)
    mix_part = sent_to_all(mix_cols, "fs_1")
    ways = []
    half_rows = mix_part.shape[0] // 2
    for way, sign in ((0, -1), (1, 1)):
        mine = mix_part[way * half_rows : (way + 1) * half_rows]
        mine, back = doubled(mine, [0], (4, 2, 1), sign)
        mine = mine.reshape(n0, n1 // 2, rows, -1)
        ways.append(jnp.stack([mine[back.index(o)] for o in offsets], axis=1))
    mix_own = jnp.concatenate(ways, axis=0).reshape(d, -1)
    mix_full = [mix_own, other_core(mix_own)]

    small = jnp.concatenate(
        [ffn_taps, ffn_bias[None], jnp.pad(mix_taps, ((0, 0), (0, hidden_w - width)))], axis=0
    )
    small = jnp.pad(small, ((0, 0), (0, main + LANES - hidden_w)))
    small = [small, other_core(small)]
    mix_taps = [s[4:7, :width] for s in small]
    extra = jnp.where(core == 0, jnp.stack(small), jnp.stack(small[::-1]))[:, :4]

    place = jnp.arange(d)
    k = place // rows % n0
    ahead = sum(jnp.where(k == i, o, 0) for i, o in enumerate(offsets))
    z = (lax.axis_index("fs_0") + ahead) % n0
    source = z * (n1 * rows) + place // (rows * n0) * rows + place % rows
    chosen = (jnp.arange(d)[:, None] == source[None, :]).astype(BF16)

    def turned(gain):
        blocks = gain.reshape(n0, n1, rows)
        twice = jnp.concatenate([blocks, blocks], axis=0)
        mine = lax.dynamic_slice_in_dim(twice, lax.axis_index("fs_0"), n0, 0)
        return jnp.stack([mine[o] for o in offsets], axis=1).reshape(-1)

    half = stream.shape[0] // 2
    stream = lax.dynamic_slice_in_dim(stream, core * half, half, 0)
    stream = dot(stream, chosen).astype(BF16)
    resid = stream.astype(F32)
    normed = norm_scale(resid, turned(mix_pre_gain)).astype(BF16)
    partial_value = 0.0
    for weights, taps in zip(mix_full, mix_taps):
        three = dot(normed, weights[:, : 3 * width]).astype(BF16).astype(F32)
        outer, inner, value = jnp.split(three, 3, axis=1)
        mixed = (outer * conv_three(inner * value, taps)).astype(BF16)
        partial_value = partial_value + dot_t(mixed, weights[:, 3 * width :])
    branch = rows_summed(partial_value)
    own_rows = branch.shape[0]
    own = lax.dynamic_slice_in_dim(stream, lax.axis_index("x") * own_rows, own_rows, 0)
    middle = own.astype(F32) + norm_scale(branch, turned(mix_post_gain))
    middle = middle.astype(BF16).astype(F32)
    normed_two = sent_to_all(norm_scale(middle, turned(ffn_pre_gain)).astype(BF16), "x")

    partial_two = ffn(normed_two, extra, ffn_full, main, tail)
    branch_two = rows_summed(partial_two)
    result = (middle + norm_scale(branch_two, turned(ffn_post_gain))).astype(BF16)
    result = sent_to_all(dot_t(result, chosen).astype(BF16), "x")
    return lax.all_gather(result, "core", axis=0, tiled=True)


def solution(mesh):
    split = Mesh(
        mesh.devices.reshape(mesh.shape["rep"], 8, 8, mesh.shape["tp"] // 2, 2),
        ("rep", "fs_0", "fs_1", "x", "core"),
    )
    return jax.shard_map(
        layer,
        mesh=split,
        in_specs=(
            P(REP_FS, None),
            P(),
            P(FS, TP),
            P(FS, TP),
            P(FS, TP),
            P(None, TP),
            P(TP, FS),
            P(),
            P(),
            P(FS, TP),
            P(FS, TP),
            P(None, TP),
            P(TP),
            P(TP, FS),
            P(),
        ),
        out_specs=P(REP_FS, None),
        check_vma=False,
    )
```

```python
import jax
import jax.numpy as jnp
from jax import lax
from jax.experimental import pallas as pl
from jax.experimental.pallas import tpu as pltpu
from jax.sharding import Mesh
from jax.sharding import PartitionSpec as P

SEQ_LEN = 128
FS = ("fs_0", "fs_1")
TP = ("x", "core")
REP_FS = ("rep", "fs_0", "fs_1")
EPS = 1e-06
F32 = jnp.float32
BF16 = jnp.bfloat16
LANES = 128
BLOCK_ROWS = 512


def from_ahead(x, steps):
    n = lax.axis_size("rep") * lax.axis_size("fs_0")
    return lax.ppermute(x, ("rep", "fs_0"), [(i, (i - steps) % n) for i in range(n)])


def doubled(x, offsets, steps, sign):
    for step in steps:
        arrived = from_ahead(x, sign * step)
        x = jnp.concatenate([x, arrived], axis=0)
        offsets = offsets + [o + sign * step for o in offsets]
    return x, [o % lax.axis_size("fs_0") for o in offsets]


def other_core(x):
    return lax.ppermute(x, "core", [(0, 1), (1, 0)])


def ffn_kernel(x_ref, extra_ref, weights_ref, out_ref, held, arrived, *, hidden_w):
    tokens, d = x_ref.shape
    blocks = d // BLOCK_ROWS
    up_w = -(-2 * hidden_w // LANES) * LANES
    down_at = 2 * hidden_w // LANES * LANES
    span = held.shape[1] - down_at
    copies = []
    for i in range(2 * blocks):
        rows = pl.ds(i * BLOCK_ROWS, BLOCK_ROWS)
        copies.append(pltpu.make_async_copy(weights_ref.at[rows], held.at[rows], arrived.at[i]))
        copies[-1].start()
    row = lax.broadcasted_iota(jnp.int32, (tokens, span), 0)
    lane = lax.broadcasted_iota(jnp.int32, (tokens, span), 1)
    total = jnp.zeros((tokens, d), F32)
    for core in range(2):
        up = jnp.zeros((tokens, up_w), F32)
        for k in range(blocks):
            copies[core * blocks + k].wait()
            x = x_ref[:, k * BLOCK_ROWS : (k + 1) * BLOCK_ROWS]
            rows = pl.ds((core * blocks + k) * BLOCK_ROWS, BLOCK_ROWS)
            up += jnp.dot(x, held[rows, :up_w], preferred_element_type=F32)
        up = up.astype(BF16).astype(F32)
        linear = up[:, :span]
        gated = pltpu.roll(up, up_w - hidden_w, 1)[:, :span]
        before = jnp.where(row == 0, 0.0, pltpu.roll(gated, 1, 0))
        after = jnp.where(row == tokens - 1, 0.0, pltpu.roll(gated, tokens - 1, 0))
        taps = extra_ref[core]
        mixed = taps[0:1] * before + taps[1:2] * gated + taps[2:3] * after + taps[3:4]
        hidden = jax.nn.gelu(mixed, approximate=True) * linear
        hidden = jnp.where(lane < hidden_w, hidden, 0.0)
        hidden = pltpu.roll(hidden, 2 * hidden_w - down_at, 1).astype(BF16)
        total += lax.dot_general(
            hidden,
            held[pl.ds(core * d, d), down_at:],
            (((1,), (1,)), ((), ())),
            preferred_element_type=F32,
        )
    out_ref[...] = total.astype(BF16)


def ffn(x, extra, weights, hidden_w):
    tokens, d = x.shape
    return pl.pallas_call(
        lambda *refs: ffn_kernel(*refs, hidden_w=hidden_w),
        out_shape=jax.ShapeDtypeStruct((tokens, d), BF16),
        in_specs=[
            pl.BlockSpec(memory_space=pltpu.VMEM),
            pl.BlockSpec(memory_space=pltpu.VMEM),
            pl.BlockSpec(memory_space=pltpu.HBM),
        ],
        out_specs=pl.BlockSpec(memory_space=pltpu.VMEM),
        scratch_shapes=[
            pltpu.VMEM(weights.shape, BF16),
            pltpu.SemaphoreType.DMA((2 * d // BLOCK_ROWS,)),
        ],
        compiler_params=pltpu.CompilerParams(vmem_limit_bytes=52 * 1024 * 1024),
        cost_estimate=pl.CostEstimate(
            flops=2 * tokens * weights.size, bytes_accessed=2 * weights.size, transcendentals=0
        ),
        name="ffn",
    )(x, extra, weights)


def norm_scale(values, gain):
    return values * lax.rsqrt(jnp.mean(values * values, axis=-1, keepdims=True) + EPS) * gain


def conv_three(values, taps):
    height, breadth = values.shape
    grouped = values.reshape(height // SEQ_LEN, SEQ_LEN, breadth)
    padded = jnp.pad(grouped, ((0, 0), (1, 1), (0, 0)))
    mixed = taps[0] * padded[:, :-2] + taps[1] * padded[:, 1:-1] + taps[2] * padded[:, 2:]
    return mixed.reshape(height, breadth)


def dot(a, b):
    return jnp.dot(a, b, preferred_element_type=F32)


def dot_t(a, b):
    return lax.dot_general(a, b, (((1,), (1,)), ((), ())), preferred_element_type=F32)


def sent_to_all(x, axis):
    n = lax.axis_size(axis)
    tiles = lax.all_to_all(jnp.broadcast_to(x[None], (n, *x.shape)), axis, 0, 0, tiled=True)
    return tiles.reshape(-1, x.shape[1])


def rows_summed(partial_value):
    n = lax.axis_size("x")
    tiles = partial_value.astype(BF16).reshape(n, -1, partial_value.shape[1])
    arrived = lax.all_to_all(tiles, "x", split_axis=0, concat_axis=0, tiled=True)
    return arrived.astype(F32).sum(axis=0).astype(BF16).astype(F32)


def layer(
    stream,
    mix_pre_gain,
    w_outer_gate,
    w_inner_gate,
    w_value,
    mix_taps,
    w_mix_out,
    mix_post_gain,
    ffn_pre_gain,
    w_linear,
    w_gated,
    ffn_taps,
    ffn_bias,
    w_down,
    ffn_post_gain,
):
    width = w_value.shape[1]
    hidden_w = w_linear.shape[1]
    rows = w_value.shape[0]
    n0, n1 = lax.axis_size("fs_0"), lax.axis_size("fs_1")
    d = stream.shape[1]
    core = lax.axis_index("core")

    spare = jnp.zeros((rows, -3 * hidden_w % LANES), BF16)
    ffn_cols = jnp.concatenate([w_linear, w_gated, w_down.T, spare], axis=1)
    ffn_part, offsets = doubled(ffn_cols, [0], (4, 2, 1), 1)
    ffn_full = lax.all_gather(ffn_part, ("core", "fs_1"), axis=0, tiled=True)

    mix_cols = jnp.concatenate([w_outer_gate, w_inner_gate, w_value, w_mix_out.T], axis=1)
    mix_part = sent_to_all(mix_cols, "fs_1")
    mix_part, near = doubled(mix_part, [0], (4,), -1)
    mix_part = mix_part.reshape(len(near), 2, -1, mix_part.shape[1])
    ways = []
    for way, sign in ((0, -1), (1, 1)):
        mine = mix_part[:, way].reshape(-1, mix_part.shape[3])
        mine, back = doubled(mine, near, (2, 1), sign)
        mine = mine.reshape(n0, n1 // 2, rows, -1)
        ways.append(jnp.stack([mine[back.index(o)] for o in offsets], axis=1))
    mix_own = jnp.concatenate(ways, axis=0).reshape(d, -1)
    mix_full = [mix_own, other_core(mix_own)]

    small = jnp.concatenate(
        [ffn_taps, ffn_bias[None], jnp.pad(mix_taps, ((0, 0), (0, hidden_w - width)))], axis=0
    )
    small = jnp.pad(small, ((0, 0), (0, -hidden_w % LANES)))
    small = [small, other_core(small)]
    mix_taps = [s[4:7, :width] for s in small]
    extra = jnp.where(core == 0, jnp.stack(small), jnp.stack(small[::-1]))[:, :4]

    place = jnp.arange(d)
    k = place // rows % n0
    ahead = sum(jnp.where(k == i, o, 0) for i, o in enumerate(offsets))
    z = (lax.axis_index("fs_0") + ahead) % n0
    source = z * (n1 * rows) + place // (rows * n0) * rows + place % rows
    chosen = (jnp.arange(d)[:, None] == source[None, :]).astype(BF16)

    def turned(gain):
        blocks = gain.reshape(n0, n1, rows)
        twice = jnp.concatenate([blocks, blocks], axis=0)
        mine = lax.dynamic_slice_in_dim(twice, lax.axis_index("fs_0"), n0, 0)
        return jnp.stack([mine[o] for o in offsets], axis=1).reshape(-1)

    half = stream.shape[0] // 2
    stream = lax.dynamic_slice_in_dim(stream, core * half, half, 0)
    stream = dot(stream, chosen).astype(BF16)
    resid = stream.astype(F32)
    normed = norm_scale(resid, turned(mix_pre_gain)).astype(BF16)
    partial_value = 0.0
    for weights, taps in zip(mix_full, mix_taps):
        three = dot(normed, weights[:, : 3 * width]).astype(BF16).astype(F32)
        outer, inner, value = jnp.split(three, 3, axis=1)
        mixed = (outer * conv_three(inner * value, taps)).astype(BF16)
        partial_value = partial_value + dot_t(mixed, weights[:, 3 * width :])
    branch = rows_summed(partial_value)
    own_rows = branch.shape[0]
    own = lax.dynamic_slice_in_dim(stream, lax.axis_index("x") * own_rows, own_rows, 0)
    middle = own.astype(F32) + norm_scale(branch, turned(mix_post_gain))
    middle = middle.astype(BF16).astype(F32)
    normed_two = sent_to_all(norm_scale(middle, turned(ffn_pre_gain)).astype(BF16), "x")

    partial_two = ffn(normed_two, extra, ffn_full, hidden_w)
    branch_two = rows_summed(partial_two)
    result = (middle + norm_scale(branch_two, turned(ffn_post_gain))).astype(BF16)
    result = sent_to_all(dot_t(result, chosen).astype(BF16), "x")
    return lax.all_gather(result, "core", axis=0, tiled=True)


def solution(mesh):
    split = Mesh(
        mesh.devices.reshape(mesh.shape["rep"], 8, 8, mesh.shape["tp"] // 2, 2),
        ("rep", "fs_0", "fs_1", "x", "core"),
    )
    return jax.shard_map(
        layer,
        mesh=split,
        in_specs=(
            P(REP_FS, None),
            P(),
            P(FS, TP),
            P(FS, TP),
            P(FS, TP),
            P(None, TP),
            P(TP, FS),
            P(),
            P(),
            P(FS, TP),
            P(FS, TP),
            P(None, TP),
            P(TP),
            P(TP, FS),
            P(),
        ),
        out_specs=P(REP_FS, None),
        check_vma=False,
    )
```
